32 devices in a mesh: ep: 16 (over z, y, x), tp: 2 (over core).
Axes of the slice: x: 2, y: 2, z: 4, core: 2. Of those that a mesh axis runs over, the one named last changes fastest.
Arguments:
- tokens: bfloat16 [256, 2048], P('ep'), may hold values from -6 to 6
- mix_gain: float32 [2048], replicated, may hold values from 0.1 to 1.9
- w_query: bfloat16 [2048, 1024], P(None, 'tp'), may hold values from -0.125 to 0.125
- w_forget: bfloat16 [2048, 1024], P(None, 'tp'), may hold values from -0.125 to 0.125
- w_input: bfloat16 [2048, 1024], P(None, 'tp'), may hold values from -0.125 to 0.125
- w_outgate: bfloat16 [2048, 1024], P(None, 'tp'), may hold values from -0.125 to 0.125
- decay_floor: float32 [1024], P('tp'), may hold values from 0 to 0.9
- head_gain: float32 [128], replicated, may hold values from 0.1 to 1.9
- prev_state: float32 [256, 8, 128, 128], P('ep', 'tp'), may hold values from -4 to 4
- w_output: bfloat16 [1024, 2048], P('tp'), may hold values from -0.1875 to 0.1875
- moe_gain: float32 [2048], replicated, may hold values from 0.1 to 1.9
- route_ids: int32 [256, 2], P('ep'), may hold values from 0 to 7, all different within a row; in each aligned block of 16 rows (0 to 15, 16 to 31, ...) at most 16 rows name the same one
- route_logits: float32 [256, 2], P('ep'), may hold values from -6 to 6
- w_exp_gate: bfloat16 [16, 2048, 1536], P('ep', None, 'tp'), may hold values from -0.125 to 0.125
- w_exp_up: bfloat16 [16, 2048, 1536], P('ep', None, 'tp'), may hold values from -0.125 to 0.125
- w_exp_down: bfloat16 [16, 1536, 2048], P('ep', 'tp'), may hold values from -0.109375 to 0.109375
Outputs:
- layer_out: bfloat16 [256, 2048], P('ep')
- new_state: float32 [256, 8, 128, 128], P('ep', 'tp')
The draws below stay inside these ranges and needn't reach their ends.
Inputs may be any that keep to these rules, and one draw needn't show every extreme that they name: `route_ids`: each row names 2 different experts; within the rows of one device no expert is named more than 16 times, and in every draw some expert is named exactly 16 times in some device's rows.
All inputs are finite; a program needn't handle non-finite values.
Results may differ from the reference program's by a relative error of at most 0.014.
Values may be sent and summed in bfloat16 or wider, within the bound.
A program may use at most 128 MiB of HBM per device.

```python
import math
import jax
import jax.numpy as jnp
import numpy as np
from jax import lax

WIDTH = 2048
HEADS = 8
HEAD_DIM = 128
MIX_WIDTH = 1024
HIDDEN_SIZE = 3072
TOP_K = 2
SEQ_DEV = 16
SEQS = 256
EXPERTS = 8
CAPACITY = 16
N_EP = 16
N_TP = 2


def level_of(stream_key, extent, cuts, least, largest):
    level = 1.0
    for dim, blocks in cuts:
        heights = jax.random.uniform(jax.random.fold_in(jax.random.fold_in(stream_key, 6), dim), (blocks,), jnp.float32, least / len(cuts), largest / len(cuts))
        level = level * jnp.repeat(jnp.exp(heights), extent[dim] // blocks).reshape((-1,) + (1,) * (len(extent) - 1 - dim))
    return level


def deal_out(stream_key, own, number, rows, count, top, limit, slope):
    ranking = jax.random.permutation(stream_key, count)
    packed, usual = load_shares(count, rows * top, limit, slope, True), load_shares(count, rows * top, limit, slope, False)
    places = jnp.arange(count)

    def named(lengths, rotation):
        used = int((lengths > 0).sum())
        fixed = max(1, used // 4)
        moved = fixed + (places - fixed + rotation * (used - fixed)) % max(1, count - fixed)
        return jnp.zeros((count,), jnp.int32).at[ranking[jnp.where(places < fixed, places, moved)]].set(jnp.asarray(lengths, jnp.int32))

    lengths = jnp.where(number % 4 == 0, named(packed, number // 4), named(usual, number - number // 4 - 1))
    mixed = jax.random.permutation(jax.random.fold_in(own, 3), count)
    source_of, taker = mixed[0:count // 2 * 2:2], mixed[1:count // 2 * 2:2]
    room = jnp.minimum(lengths[source_of] - 1, limit - lengths[taker]) // 2
    room = jnp.where((source_of == ranking[0]) | (taker == ranking[0]) | (lengths[taker] == 0), 0, jnp.maximum(room, 0))
    moved = jax.random.randint(jax.random.fold_in(own, 4), (count // 2,), 0, 1 << 20) % (room + 1)
    lengths = lengths.at[source_of].add(-moved).at[taker].add(moved)
    members = jnp.searchsorted(jnp.cumsum(lengths), jnp.arange(rows * top), side="right").astype(jnp.int32)
    listing = members.reshape(top, rows).T
    listing = listing[jax.random.permutation(jax.random.fold_in(own, 1), rows)]
    rotation = jax.random.randint(jax.random.fold_in(own, 2), (rows, 1), 0, top)
    return jnp.take_along_axis(listing, (jnp.arange(top)[None, :] + rotation) % top, axis=1)


def load_shares(amount, total, limit, lean, full):
    weights = [(1 << 20) // math.isqrt(grade ** lean) + 1 for grade in range(1, amount + 1)]
    largest = limit if full else min(limit, max(-(-total // amount), total * weights[0] // sum(weights)))
    least = 1 if total - largest >= amount - 1 else 0
    given, surplus = [largest] + [least] * (amount - 1), total - largest - least * (amount - 1)
    while surplus > 0:
        movable = [i for i in range(1, amount) if given[i] < largest] or [i for i in range(1, amount) if given[i] < limit]
        whole, remaining = sum([weights[i] for i in movable]), surplus
        for i in movable:
            addition = min(limit - given[i], max(1, remaining * weights[i] // whole), surplus)
            given[i] = given[i] + addition
            surplus = surplus - addition
    return np.array(given)


def normal_values(key, dims, spread, reach, pieces=(), held_as=jnp.bfloat16):
    array = jax.random.normal(key, dims, jnp.float32) * spread
    if len(pieces) > 0:
        array = level_of(key, dims, pieces, -0.22, 0.18) * array
    return jnp.clip(array, min=-reach, max=reach).astype(held_as)


def setup_inputs(seed: int = 0) -> dict:
    key_of = jax.random.split(jax.random.key(seed), 17)
    tokens = normal_values(key_of[0], (SEQS, WIDTH), 1.0, 6.0, ((0, 16),))
    mix_gain = jnp.clip(1.0 + 0.18 * jax.random.normal(key_of[1], (WIDTH,), jnp.float32), 0.1, 1.9)
    w_query = normal_values(key_of[2], (WIDTH, MIX_WIDTH), WIDTH ** -0.5, 0.125, ((1, 2),))
    w_forget = normal_values(key_of[3], (WIDTH, MIX_WIDTH), WIDTH ** -0.5, 0.125, ((1, 2),))
    w_input = normal_values(key_of[4], (WIDTH, MIX_WIDTH), WIDTH ** -0.5, 0.125, ((1, 2),))
    w_outgate = normal_values(key_of[5], (WIDTH, MIX_WIDTH), WIDTH ** -0.5, 0.125, ((1, 2),))
    decay_floor = jnp.clip(0.9 * jax.random.uniform(key_of[6], (MIX_WIDTH,), jnp.float32) ** level_of(key_of[6], (MIX_WIDTH,), ((0, 2),), -0.2, 0.2), 0.0, 0.9)
    head_gain = jnp.clip(1.0 + 0.18 * jax.random.normal(key_of[7], (HEAD_DIM,), jnp.float32), 0.1, 1.9)
    prev_state = normal_values(key_of[8], (SEQS, HEADS, HEAD_DIM, HEAD_DIM), 0.3, 4.0, ((0, 16), (1, 2)), jnp.float32)
    w_output = normal_values(key_of[9], (MIX_WIDTH, WIDTH), MIX_WIDTH ** -0.5, 0.1875, ((0, 2),))
    moe_gain = jnp.clip(1.0 + 0.18 * jax.random.normal(key_of[10], (WIDTH,), jnp.float32), 0.1, 1.9)
    route_ids_keys = jax.random.split(jax.random.fold_in(key_of[11], 1), SEQS // SEQ_DEV)
    route_ids_turns = jax.random.permutation(jax.random.fold_in(key_of[11], 3), SEQS // SEQ_DEV)
    route_ids = jax.vmap(lambda own, number: deal_out(jax.random.fold_in(key_of[11], 2), own, number, SEQ_DEV, EXPERTS, TOP_K, CAPACITY, 2))(route_ids_keys, route_ids_turns).reshape((SEQS, TOP_K))
    route_logits = normal_values(key_of[12], (SEQS, TOP_K), 1.5, 6.0, ((0, 16),), jnp.float32)
    w_exp_gate = normal_values(key_of[13], (2 * EXPERTS, WIDTH, HIDDEN_SIZE // 2), WIDTH ** -0.5, 0.125, ((0, 16), (2, 2)))
    w_exp_up = normal_values(key_of[14], (2 * EXPERTS, WIDTH, HIDDEN_SIZE // 2), WIDTH ** -0.5, 0.125, ((0, 16), (2, 2)))
    w_exp_down = normal_values(key_of[15], (2 * EXPERTS, HIDDEN_SIZE // 2, WIDTH), HIDDEN_SIZE ** -0.5, 0.109375, ((0, 16), (1, 2)))
    return {"tokens": tokens, "mix_gain": mix_gain, "w_query": w_query, "w_forget": w_forget, "w_input": w_input, "w_outgate": w_outgate, "decay_floor": decay_floor, "head_gain": head_gain, "prev_state": prev_state, "w_output": w_output, "moe_gain": moe_gain, "route_ids": route_ids, "route_logits": route_logits, "w_exp_gate": w_exp_gate, "w_exp_up": w_exp_up, "w_exp_down": w_exp_down}


epsilon = 1e-06

def rms_scale(values, gains):
    return values * lax.rsqrt(lax.optimization_barrier(jnp.mean(values * values, axis=-1, keepdims=True)) + epsilon) * gains

def reference(tokens, mix_gain, w_query, w_forget, w_input, w_outgate, decay_floor, head_gain, prev_state, w_output, moe_gain, route_ids, route_logits, w_exp_gate, w_exp_up, w_exp_down):
    seq_count = tokens.shape[0]
    residual = tokens.astype(jnp.float32)
    normed = rms_scale(residual, mix_gain).astype(jnp.bfloat16)
    query_part = jnp.dot(normed, w_query, preferred_element_type=jnp.float32).reshape(seq_count, HEADS, HEAD_DIM)
    forget_pre = jnp.dot(normed, w_forget, preferred_element_type=jnp.float32).reshape(seq_count, HEADS, HEAD_DIM)
    value_part = jnp.dot(normed, w_input, preferred_element_type=jnp.float32).reshape(seq_count, HEADS, HEAD_DIM)
    outgate_pre = jnp.dot(normed, w_outgate, preferred_element_type=jnp.float32).reshape(seq_count, HEADS, HEAD_DIM)
    floor_rate = decay_floor.reshape(HEADS, HEAD_DIM)
    forget = floor_rate + (1.0 - floor_rate) * jax.nn.sigmoid(forget_pre)
    key_part = (1.0 - floor_rate) * jax.nn.sigmoid(-forget_pre)
    new_state = forget[..., None] * prev_state + key_part[..., None] * value_part[:, :, None, :]
    readout = lax.optimization_barrier(jnp.sum(query_part[..., None] * new_state, axis=2))
    gated = (rms_scale(readout, head_gain) * jax.nn.silu(outgate_pre)).reshape(seq_count, MIX_WIDTH).astype(jnp.bfloat16)
    head_width = MIX_WIDTH // N_TP
    mixed_out = jnp.zeros((seq_count, WIDTH), jnp.float32)
    for part_index in range(N_TP):
        lower = part_index * head_width
        partial_out = jnp.dot(gated[:, lower:lower + head_width], w_output[lower:lower + head_width], preferred_element_type=jnp.float32).astype(jnp.bfloat16)
        mixed_out = mixed_out + lax.optimization_barrier(partial_out).astype(jnp.float32)
    middle = (residual + mixed_out).astype(jnp.bfloat16)
    normed_two = rms_scale(middle.astype(jnp.float32), moe_gain).astype(jnp.bfloat16)
    pair_expert = route_ids.reshape(-1).astype(jnp.int32)
    pair_count = pair_expert.shape[0]
    onehot = (pair_expert[:, None] == jnp.arange(EXPERTS, dtype=jnp.int32)[None, :]).astype(jnp.int32)
    slot_rank = lax.optimization_barrier(jnp.sum((jnp.cumsum(onehot, axis=0) - onehot) * onehot, axis=1)).astype(jnp.int32)
    slot_limit = N_EP * CAPACITY
    slot_table = jnp.zeros((EXPERTS, slot_limit), jnp.int32).at[pair_expert, slot_rank].set(jnp.arange(pair_count, dtype=jnp.int32) // TOP_K)
    half_hidden = w_exp_gate.shape[2]
    piece_hidden = half_hidden // N_TP

    def half_expert(half_index):
        slot_rows = normed_two[slot_table[half_index // 2]]
        gate_pre = jnp.dot(slot_rows, w_exp_gate[half_index], preferred_element_type=jnp.float32)
        up_pre = jnp.dot(slot_rows, w_exp_up[half_index], preferred_element_type=jnp.float32)
        activated = (jax.nn.silu(gate_pre) * up_pre).astype(jnp.bfloat16)
        down_all = w_exp_down[half_index]
        running = jnp.zeros((slot_limit, WIDTH), jnp.float32)
        for part_index in range(N_TP):
            lower = part_index * piece_hidden
            partial_down = jnp.dot(activated[:, lower:lower + piece_hidden], down_all[lower:lower + piece_hidden], preferred_element_type=jnp.float32).astype(jnp.bfloat16)
            running = running + lax.optimization_barrier(partial_down).astype(jnp.float32)
        return running.astype(jnp.bfloat16)
    halves = lax.map(half_expert, jnp.arange(2 * EXPERTS, dtype=jnp.int32))
    first_half = halves[2 * pair_expert, slot_rank].astype(jnp.float32)
    second = halves[2 * pair_expert + 1, slot_rank].astype(jnp.float32)
    both_halves = (first_half + second).reshape(seq_count, TOP_K, WIDTH)
    weights = jax.nn.sigmoid(route_logits - jnp.flip(route_logits, axis=1))
    expert_sum = lax.optimization_barrier(jnp.sum(weights[..., None] * both_halves, axis=1))
    layer_out = (middle.astype(jnp.float32) + expert_sum).astype(jnp.bfloat16)
    return (layer_out, new_state)
```

```python
import functools

import jax
import jax.numpy as jnp
from jax import lax
from jax.experimental import pallas as pl
from jax.experimental.pallas import tpu as pltpu
from jax.sharding import PartitionSpec as P

epsilon = 1e-06
LANES = 128
MESH = pl.DeviceIdType.MESH


def rms_scale(values, gains):
    return values * lax.rsqrt(jnp.mean(values * values, axis=-1, keepdims=True) + epsilon) * gains


def line_size(ep_size):
    size = 1
    while size * size * size < ep_size:
        size *= 2
    return size


def moe_kernel(
    line,
    plane,
    tokens,
    partial_mix,
    moe_gain,
    route_ids,
    route_logits,
    gate_hbm,
    up_hbm,
    down_hbm,
    out,
    other_mix,
    middle,
    rows_all,
    w_gate,
    w_up,
    w_down,
    activated,
    row_weight,
    own_half,
    pair_send,
    pair_recv,
    plane_send,
    plane_recv,
    line_send,
    line_recv,
    final_half,
    w_sems,
    mix_sems,
    ag_line_send,
    ag_line_recv,
    ag_plane_send,
    ag_plane_recv,
    ag_pair_send,
    ag_pair_recv,
    rs_pair_send,
    rs_pair_recv,
    rs_plane_send,
    rs_plane_recv,
    rs_line_send,
    rs_line_recv,
    final_sems,
):
    ep_size = line * plane
    experts = ep_size // 2
    seq_dev, width = tokens.shape
    half = width // 2
    hidden = w_gate.shape[1]
    me = lax.axis_index("ep")
    core = lax.axis_index("tp")
    peer = 1 - core
    z = me // plane
    q = me % plane

    loads = [
        pltpu.make_async_copy(gate_hbm.at[0], w_gate, w_sems.at[0]),
        pltpu.make_async_copy(up_hbm.at[0], w_up, w_sems.at[1]),
        pltpu.make_async_copy(down_hbm.at[0, :, pl.ds(0, half)], w_down.at[0], w_sems.at[2]),
        pltpu.make_async_copy(down_hbm.at[0, :, pl.ds(half, half)], w_down.at[1], w_sems.at[3]),
    ]

    def at_line(dz):
        return ((z + dz) % line) * plane + q

    def at_plane(p):
        return z * plane + (q + p) % plane

    barrier = pltpu.get_barrier_semaphore()
    pl.semaphore_signal(barrier, inc=1, device_id=(me, peer), device_id_type=MESH)
    for dz in range(1, line):
        pl.semaphore_signal(barrier, inc=1, device_id=(at_line(dz), core), device_id_type=MESH)
    for p in range(1, plane):
        pl.semaphore_signal(barrier, inc=1, device_id=(at_plane(p), core), device_id_type=MESH)
    for load in loads:
        load.start()
    pl.semaphore_wait(barrier, line + plane - 1)

    def remote(src, dst, send, recv, where):
        return pltpu.make_async_remote_copy(
            src_ref=src, dst_ref=dst, send_sem=send, recv_sem=recv, device_id=where, device_id_type=MESH
        )

    mix_copy = remote(partial_mix, other_mix, mix_sems.at[0], mix_sems.at[1], (me, peer))
    mix_copy.start()

    ids = route_ids[...]
    logits = route_logits[...]
    share = jax.nn.sigmoid(logits[:, 0:1] - logits[:, 1:2])
    share_two = jax.nn.sigmoid(logits[:, 1:2] - logits[:, 0:1])
    lane = lax.broadcasted_iota(jnp.int32, (seq_dev, LANES), 1)
    slot = lane % experts
    coef = jnp.where(ids[:, 0:1] == slot, share, 0.0) + jnp.where(ids[:, 1:2] == slot, share_two, 0.0)
    coef_high = coef.astype(jnp.bfloat16).astype(jnp.float32)
    coef = jnp.where(lane < experts, coef_high, coef - coef_high)
    coef = jnp.where(lane < 2 * experts, coef, 0.0)

    mix_copy.wait()
    mixed = partial_mix[...].astype(jnp.float32) + other_mix[...].astype(jnp.float32)
    mid = (tokens[...].astype(jnp.float32) + mixed).astype(jnp.bfloat16).astype(jnp.float32)
    middle[0] = mid[:, :half]
    middle[1] = mid[:, half:]
    normed = rms_scale(mid, moe_gain[...]).astype(jnp.bfloat16)
    rows_all[0, me, :, :half] = normed[:, :half]
    rows_all[1, me, :, :half] = normed[:, half:]
    for c in range(2):
        rows_all[c, me, :, half:] = coef.astype(jnp.bfloat16)

    line_copies = []
    for dz in range(line - 1, 0, -1):
        block = rows_all.at[core, me]
        cp = remote(block, block, ag_line_send.at[dz], ag_line_recv.at[dz], (at_line(dz), core))
        cp.start()
        line_copies.append((dz, cp))
    line_of = dict(line_copies)
    plane_copies = {}
    pair_copies = {}

    def hand_over(p, dz):
        source = ((z - dz + line) % line) * plane + (q - p + plane) % plane
        block = rows_all.at[core, source]
        cp = remote(block, block, ag_pair_send.at[p, dz], ag_pair_recv.at[p, dz], (me, peer))
        cp.start()
        pair_copies[p, dz] = cp

    for dz in range(line):
        if dz:
            line_of[dz].wait_recv()
        block = rows_all.at[core, ((z - dz + line) % line) * plane + q]
        for p in range(1, plane):
            cp = remote(
                block, block, ag_plane_send.at[p, dz], ag_plane_recv.at[p, dz], (at_plane(p), core)
            )
            cp.start()
            plane_copies[p, dz] = cp
        if dz:
            hand_over(0, dz)
    for dz in range(line):
        for p in range(1, plane):
            plane_copies[p, dz].wait_recv()
            hand_over(p, dz)
    for load in loads[:2]:
        load.wait()
    for key in pair_copies:
        pair_copies[key].wait_recv()

    total = ep_size * seq_dev
    chunk = min(total, 256)
    devs = chunk // seq_dev
    tile = 256 if hidden % 256 == 0 else hidden
    expert = me // 2

    @pl.loop(0, total // chunk)
    def _(m):
        rows = pl.ds(pl.multiple_of(m * chunk, chunk), chunk)
        who = pl.ds(m * devs, devs)
        sent = rows_all[0, who, :, half:].reshape(chunk, LANES).astype(jnp.float32)
        at = lax.broadcasted_iota(jnp.int32, (chunk, LANES), 1)
        picked = jnp.where((at == expert) | (at == expert + experts), sent, 0.0)
        row_weight[rows, :] = jnp.broadcast_to(
            jnp.sum(picked, axis=1, keepdims=True), (chunk, LANES)
        )

        @pl.loop(0, hidden // tile)
        def _(n):
            cols = pl.ds(pl.multiple_of(n * tile, tile), tile)
            left = rows_all[0, who, :, :half].reshape(chunk, half)
            right = rows_all[1, who, :, :half].reshape(chunk, half)
            gate = jnp.dot(left, w_gate[:half, cols], preferred_element_type=jnp.float32)
            gate += jnp.dot(right, w_gate[half:, cols], preferred_element_type=jnp.float32)
            up = jnp.dot(left, w_up[:half, cols], preferred_element_type=jnp.float32)
            up += jnp.dot(right, w_up[half:, cols], preferred_element_type=jnp.float32)
            activated[rows, cols] = (jax.nn.silu(gate) * up).astype(jnp.bfloat16)

    for load in loads[2:]:
        load.wait()
    step = 256 if half % 256 == 0 else half

    def down(which, store):
        @pl.loop(0, total // chunk)
        def _(m):
            rows = pl.ds(pl.multiple_of(m * chunk, chunk), chunk)
            who = pl.ds(m * devs, devs)

            @pl.loop(0, half // step)
            def _(n):
                cols = pl.ds(pl.multiple_of(n * step, step), step)
                value = jnp.dot(
                    activated[rows, :], w_down[which, :, cols], preferred_element_type=jnp.float32
                )
                value = value * row_weight[rows, 0:1]
                store[who, :, cols] = value.reshape(devs, seq_dev, step).astype(store.dtype)

    down(peer, pair_send)
    rs_pair = {}
    order = list(range(1, line)) + [0]
    for dz in order:
        part = pl.ds(((z + dz) % line) * plane, plane)
        cp = remote(
            pair_send.at[part], pair_recv.at[part], rs_pair_send.at[dz], rs_pair_recv.at[dz], (me, peer)
        )
        cp.start()
        rs_pair[dz] = cp
    down(core, own_half)

    rs_plane = {}
    for dz in order:
        first = ((z + dz) % line) * plane
        part = pl.ds(first, plane)
        rs_pair[dz].wait_recv()
        joined = own_half[part] + pair_recv[part].astype(jnp.float32)
        own_half[part] = joined
        plane_send[dz] = joined.astype(jnp.bfloat16)
        for p in range(1, plane):
            cp = remote(
                plane_send.at[dz, (q + p) % plane],
                plane_recv.at[dz, p],
                rs_plane_send.at[p, dz],
                rs_plane_recv.at[p, dz],
                (at_plane(p), core),
            )
            cp.start()
            rs_plane[p, dz] = cp
    rs_line = {}
    kept = None
    for dz in order:
        block = own_half[((z + dz) % line) * plane + q]
        for p in range(1, plane):
            rs_plane[p, dz].wait_recv()
            block = block + plane_recv[dz, p].astype(jnp.float32)
        if dz:
            line_send[dz] = block.astype(jnp.bfloat16)
            cp = remote(
                line_send.at[dz],
                line_recv.at[dz],
                rs_line_send.at[dz],
                rs_line_recv.at[dz],
                (at_line(dz), core),
            )
            cp.start()
            rs_line[dz] = cp
        else:
            kept = block
    for dz in range(1, line):
        rs_line[dz].wait_recv()
        kept = kept + line_recv[dz].astype(jnp.float32)
    final_half[core] = (middle[core] + kept).astype(jnp.bfloat16)
    last = remote(
        final_half.at[core], final_half.at[core], final_sems.at[0], final_sems.at[1], (me, peer)
    )
    last.start()
    for copies in (line_of, plane_copies, pair_copies, rs_pair, rs_plane, rs_line):
        for key in copies:
            copies[key].wait_send()
    last.wait()
    out[:, :half] = final_half[0]
    out[:, half:] = final_half[1]


def moe(tokens, partial_mix, moe_gain, route_ids, route_logits, w_gate, w_up, w_down):
    seq_dev, width = tokens.shape
    half = width // 2
    hidden = w_gate.shape[2]
    ep_size = lax.axis_size("ep")
    line = line_size(ep_size)
    plane = ep_size // line
    bf, f32 = jnp.bfloat16, jnp.float32
    dma = pltpu.SemaphoreType.DMA
    vmem = pl.BlockSpec(memory_space=pltpu.VMEM)
    hbm = pl.BlockSpec(memory_space=pl.ANY)
    return pl.pallas_call(
        functools.partial(moe_kernel, line, plane),
        out_shape=jax.ShapeDtypeStruct((seq_dev, width), bf),
        in_specs=[vmem] * 5 + [hbm] * 3,
        out_specs=vmem,
        scratch_shapes=[
            pltpu.VMEM((seq_dev, width), bf),
            pltpu.VMEM((2, seq_dev, half), f32),
            pltpu.VMEM((2, ep_size, seq_dev, half + LANES), bf),
            pltpu.VMEM((width, hidden), bf),
            pltpu.VMEM((width, hidden), bf),
            pltpu.VMEM((2, hidden, half), bf),
            pltpu.VMEM((ep_size * seq_dev, hidden), bf),
            pltpu.VMEM((ep_size * seq_dev, LANES), f32),
            pltpu.VMEM((ep_size, seq_dev, half), f32),
            pltpu.VMEM((ep_size, seq_dev, half), bf),
            pltpu.VMEM((ep_size, seq_dev, half), bf),
            pltpu.VMEM((line, plane, seq_dev, half), bf),
            pltpu.VMEM((line, plane, seq_dev, half), bf),
            pltpu.VMEM((line, seq_dev, half), bf),
            pltpu.VMEM((line, seq_dev, half), bf),
            pltpu.VMEM((2, seq_dev, half), bf),
            dma((4,)),
            dma((2,)),
            dma((line,)),
            dma((line,)),
            dma((plane, line)),
            dma((plane, line)),
            dma((plane, line)),
            dma((plane, line)),
            dma((line,)),
            dma((line,)),
            dma((plane, line)),
            dma((plane, line)),
            dma((line,)),
            dma((line,)),
            dma((2,)),
        ],
        compiler_params=pltpu.CompilerParams(
            collective_id=0, has_side_effects=True, vmem_limit_bytes=60 * 1024 * 1024
        ),
        name="moe",
    )(tokens, partial_mix, moe_gain.reshape(1, width), route_ids, route_logits, w_gate, w_up, w_down)


def on_device(
    tokens,
    mix_gain,
    w_query,
    w_forget,
    w_input,
    w_outgate,
    decay_floor,
    head_gain,
    prev_state,
    w_output,
    moe_gain,
    route_ids,
    route_logits,
    w_exp_gate,
    w_exp_up,
    w_exp_down,
):
    seq_dev = tokens.shape[0]
    residual = tokens.astype(jnp.float32)
    normed = rms_scale(residual, mix_gain).astype(jnp.bfloat16)
    heads_dev = prev_state.shape[1]
    head_dim = prev_state.shape[2]
    head_width = heads_dev * head_dim

    def project(weight):
        return jnp.dot(normed, weight, preferred_element_type=jnp.float32).reshape(
            seq_dev, heads_dev, head_dim
        )

    query_part, forget_pre = project(w_query), project(w_forget)
    value_part, outgate_pre = project(w_input), project(w_outgate)
    floor_rate = decay_floor.reshape(heads_dev, head_dim)
    forget = floor_rate + (1.0 - floor_rate) * jax.nn.sigmoid(forget_pre)
    key_part = (1.0 - floor_rate) * jax.nn.sigmoid(-forget_pre)
    new_state = forget[..., None] * prev_state + key_part[..., None] * value_part[:, :, None, :]
    readout = jnp.sum(query_part[..., None] * new_state, axis=2)
    gated = (
        (rms_scale(readout, head_gain) * jax.nn.silu(outgate_pre))
        .reshape(seq_dev, head_width)
        .astype(jnp.bfloat16)
    )
    partial_mix = jnp.dot(gated, w_output, preferred_element_type=jnp.float32).astype(jnp.bfloat16)
    layer_out = moe(
        tokens, partial_mix, moe_gain, route_ids, route_logits, w_exp_gate, w_exp_up, w_exp_down
    )
    return (layer_out, new_state)


def solution(mesh):
    placed = (
        P("ep", None),
        P(),
        P(None, "tp"),
        P(None, "tp"),
        P(None, "tp"),
        P(None, "tp"),
        P("tp"),
        P(),
        P("ep", "tp", None, None),
        P("tp", None),
        P(),
        P("ep", None),
        P("ep", None),
        P("ep", None, "tp"),
        P("ep", None, "tp"),
        P("ep", "tp", None),
    )
    return jax.shard_map(
        on_device,
        mesh=mesh,
        in_specs=placed,
        out_specs=(P("ep", None), P("ep", "tp", None, None)),
        check_vma=False,
    )
```

```python
import functools

import jax
import jax.numpy as jnp
from jax import lax
from jax.experimental import pallas as pl
from jax.experimental.pallas import tpu as pltpu
from jax.sharding import PartitionSpec as P

epsilon = 1e-06
LANES = 128
MESH = pl.DeviceIdType.MESH


def rms_scale(values, gains):
    return values * lax.rsqrt(jnp.mean(values * values, axis=-1, keepdims=True) + epsilon) * gains


def line_size(ep_size):
    size = 1
    while size * size * size < ep_size:
        size *= 2
    return size


def moe_kernel(
    line,
    plane,
    tokens,
    partial_mix,
    moe_gain,
    coef,
    gate_hbm,
    up_hbm,
    down_hbm,
    out,
    other_mix,
    middle,
    rows_all,
    w_gate,
    w_up,
    w_down,
    activated,
    row_weight,
    own_half,
    pair_send,
    pair_recv,
    plane_send,
    plane_recv,
    line_send,
    line_recv,
    final_half,
    w_sems,
    mix_sems,
    ag_line_send,
    ag_line_recv,
    ag_plane_send,
    ag_plane_recv,
    ag_pair_send,
    ag_pair_recv,
    rs_pair_send,
    rs_pair_recv,
    rs_plane_send,
    rs_plane_recv,
    rs_line_send,
    rs_line_recv,
    final_sems,
):
    ep_size = line * plane
    experts = ep_size // 2
    seq_dev, width = tokens.shape
    half = width // 2
    hidden = w_gate.shape[1]
    me = lax.axis_index("ep")
    core = lax.axis_index("tp")
    peer = 1 - core
    z = me // plane
    q = me % plane

    loads = [
        pltpu.make_async_copy(gate_hbm.at[0], w_gate, w_sems.at[0]),
        pltpu.make_async_copy(up_hbm.at[0], w_up, w_sems.at[1]),
        pltpu.make_async_copy(down_hbm.at[0, :, pl.ds(0, half)], w_down.at[0], w_sems.at[2]),
        pltpu.make_async_copy(down_hbm.at[0, :, pl.ds(half, half)], w_down.at[1], w_sems.at[3]),
    ]

    def at_line(dz):
        return ((z + dz) % line) * plane + q

    def at_plane(p):
        return z * plane + (q + p) % plane

    barrier = pltpu.get_barrier_semaphore()
    pl.semaphore_signal(barrier, inc=1, device_id=(me, peer), device_id_type=MESH)
    for dz in range(1, line):
        pl.semaphore_signal(barrier, inc=1, device_id=(at_line(dz), core), device_id_type=MESH)
    for p in range(1, plane):
        pl.semaphore_signal(barrier, inc=1, device_id=(at_plane(p), core), device_id_type=MESH)
    for load in loads:
        load.start()
    pl.semaphore_wait(barrier, line + plane - 1)

    def remote(src, dst, send, recv, where):
        return pltpu.make_async_remote_copy(
            src_ref=src, dst_ref=dst, send_sem=send, recv_sem=recv, device_id=where, device_id_type=MESH
        )

    mix_copy = remote(partial_mix, other_mix, mix_sems.at[0], mix_sems.at[1], (me, peer))
    mix_copy.start()

    mix_copy.wait()
    mixed = partial_mix[...].astype(jnp.float32) + other_mix[...].astype(jnp.float32)
    mid = (tokens[...].astype(jnp.float32) + mixed).astype(jnp.bfloat16).astype(jnp.float32)
    middle[0] = mid[:, :half]
    middle[1] = mid[:, half:]
    normed = rms_scale(mid, moe_gain[...]).astype(jnp.bfloat16)
    rows_all[0, me, :, :half] = normed[:, :half]
    rows_all[1, me, :, :half] = normed[:, half:]
    for c in range(2):
        rows_all[c, me, :, half:] = coef[...]

    line_copies = []
    for dz in range(line - 1, 0, -1):
        block = rows_all.at[core, me]
        cp = remote(block, block, ag_line_send.at[dz], ag_line_recv.at[dz], (at_line(dz), core))
        cp.start()
        line_copies.append((dz, cp))
    line_of = dict(line_copies)
    plane_copies = {}
    pair_copies = {}

    def hand_over(p, dz):
        source = ((z - dz + line) % line) * plane + (q - p + plane) % plane
        block = rows_all.at[core, source]
        cp = remote(block, block, ag_pair_send.at[p, dz], ag_pair_recv.at[p, dz], (me, peer))
        cp.start()
        pair_copies[p, dz] = cp

    for dz in range(line):
        if dz:
            line_of[dz].wait_recv()
        block = rows_all.at[core, ((z - dz + line) % line) * plane + q]
        for p in range(1, plane):
            cp = remote(
                block, block, ag_plane_send.at[p, dz], ag_plane_recv.at[p, dz], (at_plane(p), core)
            )
            cp.start()
            plane_copies[p, dz] = cp
        if dz:
            hand_over(0, dz)
    for dz in range(line):
        for p in range(1, plane):
            plane_copies[p, dz].wait_recv()
            hand_over(p, dz)
    for load in loads[:2]:
        load.wait()
    for key in pair_copies:
        pair_copies[key].wait_recv()

    total = ep_size * seq_dev
    chunk = min(total, 256)
    devs = chunk // seq_dev
    tile = 256 if hidden % 256 == 0 else hidden
    expert = me // 2

    @pl.loop(0, total // chunk)
    def _(m):
        rows = pl.ds(pl.multiple_of(m * chunk, chunk), chunk)
        who = pl.ds(m * devs, devs)
        sent = rows_all[0, who, :, half:].reshape(chunk, LANES).astype(jnp.float32)
        at = lax.broadcasted_iota(jnp.int32, (chunk, LANES), 1)
        picked = jnp.where((at == expert) | (at == expert + experts), sent, 0.0)
        row_weight[rows, :] = jnp.broadcast_to(
            jnp.sum(picked, axis=1, keepdims=True), (chunk, LANES)
        )

        @pl.loop(0, hidden // tile)
        def _(n):
            cols = pl.ds(pl.multiple_of(n * tile, tile), tile)
            left = rows_all[0, who, :, :half].reshape(chunk, half)
            right = rows_all[1, who, :, :half].reshape(chunk, half)
            gate = jnp.dot(left, w_gate[:half, cols], preferred_element_type=jnp.float32)
            gate += jnp.dot(right, w_gate[half:, cols], preferred_element_type=jnp.float32)
            up = jnp.dot(left, w_up[:half, cols], preferred_element_type=jnp.float32)
            up += jnp.dot(right, w_up[half:, cols], preferred_element_type=jnp.float32)
            activated[rows, cols] = (jax.nn.silu(gate) * up).astype(jnp.bfloat16)

    for load in loads[2:]:
        load.wait()
    step = 256 if half % 256 == 0 else half

    def down(which, store):
        @pl.loop(0, total // chunk)
        def _(m):
            rows = pl.ds(pl.multiple_of(m * chunk, chunk), chunk)
            who = pl.ds(m * devs, devs)

            @pl.loop(0, half // step)
            def _(n):
                cols = pl.ds(pl.multiple_of(n * step, step), step)
                value = jnp.dot(
                    activated[rows, :], w_down[which, :, cols], preferred_element_type=jnp.float32
                )
                value = value * row_weight[rows, 0:1]
                store[who, :, cols] = value.reshape(devs, seq_dev, step).astype(store.dtype)

    down(peer, pair_send)
    rs_pair = {}
    order = list(range(1, line)) + [0]
    for dz in order:
        part = pl.ds(((z + dz) % line) * plane, plane)
        cp = remote(
            pair_send.at[part], pair_recv.at[part], rs_pair_send.at[dz], rs_pair_recv.at[dz], (me, peer)
        )
        cp.start()
        rs_pair[dz] = cp
    down(core, own_half)

    rs_plane = {}
    for dz in order:
        first = ((z + dz) % line) * plane
        part = pl.ds(first, plane)
        rs_pair[dz].wait_recv()
        joined = own_half[part] + pair_recv[part].astype(jnp.float32)
        own_half[part] = joined
        plane_send[dz] = joined.astype(jnp.bfloat16)
        for p in range(1, plane):
            cp = remote(
                plane_send.at[dz, (q + p) % plane],
                plane_recv.at[dz, p],
                rs_plane_send.at[p, dz],
                rs_plane_recv.at[p, dz],
                (at_plane(p), core),
            )
            cp.start()
            rs_plane[p, dz] = cp
    rs_line = {}
    kept = None
    for dz in order:
        block = own_half[((z + dz) % line) * plane + q]
        for p in range(1, plane):
            rs_plane[p, dz].wait_recv()
            block = block + plane_recv[dz, p].astype(jnp.float32)
        if dz:
            line_send[dz] = block.astype(jnp.bfloat16)
            cp = remote(
                line_send.at[dz],
                line_recv.at[dz],
                rs_line_send.at[dz],
                rs_line_recv.at[dz],
                (at_line(dz), core),
            )
            cp.start()
            rs_line[dz] = cp
        else:
            kept = block
    for dz in range(1, line):
        rs_line[dz].wait_recv()
        kept = kept + line_recv[dz].astype(jnp.float32)
    final_half[core] = (middle[core] + kept).astype(jnp.bfloat16)
    last = remote(
        final_half.at[core], final_half.at[core], final_sems.at[0], final_sems.at[1], (me, peer)
    )
    last.start()
    for copies in (line_of, plane_copies, pair_copies, rs_pair, rs_plane, rs_line):
        for key in copies:
            copies[key].wait_send()
    last.wait()
    out[:, :half] = final_half[0]
    out[:, half:] = final_half[1]


def moe(tokens, partial_mix, moe_gain, coef, w_gate, w_up, w_down):
    seq_dev, width = tokens.shape
    half = width // 2
    hidden = w_gate.shape[2]
    ep_size = lax.axis_size("ep")
    line = line_size(ep_size)
    plane = ep_size // line
    bf, f32 = jnp.bfloat16, jnp.float32
    dma = pltpu.SemaphoreType.DMA
    vmem = pl.BlockSpec(memory_space=pltpu.VMEM)
    hbm = pl.BlockSpec(memory_space=pl.ANY)
    return pl.pallas_call(
        functools.partial(moe_kernel, line, plane),
        out_shape=jax.ShapeDtypeStruct((seq_dev, width), bf),
        in_specs=[vmem] * 4 + [hbm] * 3,
        out_specs=vmem,
        scratch_shapes=[
            pltpu.VMEM((seq_dev, width), bf),
            pltpu.VMEM((2, seq_dev, half), f32),
            pltpu.VMEM((2, ep_size, seq_dev, half + LANES), bf),
            pltpu.VMEM((width, hidden), bf),
            pltpu.VMEM((width, hidden), bf),
            pltpu.VMEM((2, hidden, half), bf),
            pltpu.VMEM((ep_size * seq_dev, hidden), bf),
            pltpu.VMEM((ep_size * seq_dev, LANES), f32),
            pltpu.VMEM((ep_size, seq_dev, half), f32),
            pltpu.VMEM((ep_size, seq_dev, half), bf),
            pltpu.VMEM((ep_size, seq_dev, half), bf),
            pltpu.VMEM((line, plane, seq_dev, half), bf),
            pltpu.VMEM((line, plane, seq_dev, half), bf),
            pltpu.VMEM((line, seq_dev, half), bf),
            pltpu.VMEM((line, seq_dev, half), bf),
            pltpu.VMEM((2, seq_dev, half), bf),
            dma((4,)),
            dma((2,)),
            dma((line,)),
            dma((line,)),
            dma((plane, line)),
            dma((plane, line)),
            dma((plane, line)),
            dma((plane, line)),
            dma((line,)),
            dma((line,)),
            dma((plane, line)),
            dma((plane, line)),
            dma((line,)),
            dma((line,)),
            dma((2,)),
        ],
        compiler_params=pltpu.CompilerParams(
            collective_id=0, has_side_effects=True, vmem_limit_bytes=60 * 1024 * 1024
        ),
        name="moe",
    )(tokens, partial_mix, moe_gain.reshape(1, width), coef, w_gate, w_up, w_down)


def mix_kernel(
    experts,
    tokens,
    mix_gain,
    floors,
    head_gain,
    ids,
    logits,
    query_hbm,
    forget_hbm,
    input_hbm,
    outgate_hbm,
    prev_hbm,
    output_hbm,
    partial_mix,
    coef,
    state_hbm,
    weights,
    state,
    w_output,
    columns,
    readout,
    total,
    w_sems,
    in_sems,
    out_sems,
    last_sem,
):
    groups = weights.shape[1]
    span = weights.shape[3]
    seq_dev = tokens.shape[0]
    heads_dev, head_dim = floors.shape
    per_group = heads_dev // groups
    loads, states, stores = {}, [], []
    for g in range(groups):
        cols = pl.ds(g * span, span)
        for n, source in enumerate((forget_hbm, query_hbm, input_hbm, outgate_hbm)):
            loads[n, g] = pltpu.make_async_copy(source.at[:, cols], weights.at[n, g], w_sems.at[n, g])
            loads[n, g].start()
        for h in range(g * per_group, (g + 1) * per_group):
            cp = pltpu.make_async_copy(prev_hbm.at[:, h], state.at[h], in_sems.at[h])
            cp.start()
            states.append(cp)
            stores.append(pltpu.make_async_copy(state.at[h], state_hbm.at[:, h], out_sems.at[h]))
    last = pltpu.make_async_copy(output_hbm, w_output, last_sem)
    last.start()

    slot = lax.broadcasted_iota(jnp.int32, (LANES, seq_dev), 0)
    named = slot % experts
    share = jax.nn.sigmoid(logits[0:1, :] - logits[1:2, :])
    share_two = jax.nn.sigmoid(logits[1:2, :] - logits[0:1, :])
    value = jnp.where(ids[0:1, :] == named, share, 0.0) + jnp.where(ids[1:2, :] == named, share_two, 0.0)
    high = value.astype(jnp.bfloat16).astype(jnp.float32)
    value = jnp.where(slot < experts, high, value - high)
    value = jnp.where(slot < 2 * experts, value, 0.0)
    value = jnp.concatenate([value, jnp.zeros((LANES, LANES - seq_dev), jnp.float32)], axis=1)
    coef[...] = value.T[:seq_dev].astype(jnp.bfloat16)

    normed = rms_scale(tokens[...].astype(jnp.float32), mix_gain[...]).astype(jnp.bfloat16)
    fill = jnp.zeros((head_dim - 3 * seq_dev, head_dim), jnp.float32)
    for g in range(groups):

        def project(n):
            loads[n, g].wait()
            return jnp.dot(normed, weights[n, g], preferred_element_type=jnp.float32)

        forget_pre, query, inputs, outgate_pre = [project(n) for n in range(4)]
        for k in range(per_group):
            h = g * per_group + k
            cut = slice(k * head_dim, (k + 1) * head_dim)
            floor = floors[h : h + 1, :]
            forget = floor + (1.0 - floor) * jax.nn.sigmoid(forget_pre[:, cut])
            key = (1.0 - floor) * jax.nn.sigmoid(-forget_pre[:, cut])
            columns[h] = jnp.concatenate([forget, key, query[:, cut], fill], axis=0).T
            states[h].wait()
            for s in range(seq_dev):
                fresh = (
                    columns[h, :, s : s + 1] * state[h, s]
                    + columns[h, :, seq_dev + s : seq_dev + s + 1] * inputs[s : s + 1, cut]
                )
                state[h, s] = fresh
                asked = columns[h, :, 2 * seq_dev + s : 2 * seq_dev + s + 1]
                readout[h, s : s + 1, :] = jnp.sum(asked * fresh, axis=0, keepdims=True)
            stores[h].start()
            gated = rms_scale(readout[h], head_gain[...]) * jax.nn.silu(outgate_pre[:, cut])
            total[:, h * head_dim : (h + 1) * head_dim] = gated.astype(jnp.bfloat16)
    last.wait()
    partial_mix[...] = jnp.dot(
        total[...], w_output[...], preferred_element_type=jnp.float32
    ).astype(jnp.bfloat16)
    for store in stores:
        store.wait()


def mix(
    tokens, mix_gain, decay_floor, head_gain, route_ids, route_logits, weights, prev_state, w_output, experts
):
    seq_dev, width = tokens.shape
    _, heads_dev, head_dim, _ = prev_state.shape
    head_width = heads_dev * head_dim
    groups = max(1, heads_dev // 2)
    bf, f32 = jnp.bfloat16, jnp.float32
    dma = pltpu.SemaphoreType.DMA
    vmem = pl.BlockSpec(memory_space=pltpu.VMEM)
    hbm = pl.BlockSpec(memory_space=pl.ANY)
    return pl.pallas_call(
        functools.partial(mix_kernel, experts),
        out_shape=(
            jax.ShapeDtypeStruct((seq_dev, width), bf),
            jax.ShapeDtypeStruct((seq_dev, LANES), bf),
            jax.ShapeDtypeStruct(prev_state.shape, f32),
        ),
        in_specs=[vmem] * 6 + [hbm] * 6,
        out_specs=(vmem, vmem, hbm),
        scratch_shapes=[
            pltpu.VMEM((4, groups, width, head_width // groups), bf),
            pltpu.VMEM((heads_dev, seq_dev, head_dim, head_dim), f32),
            pltpu.VMEM((head_width, width), bf),
            pltpu.VMEM((heads_dev, head_dim, head_dim), f32),
            pltpu.VMEM((heads_dev, seq_dev, head_dim), f32),
            pltpu.VMEM((seq_dev, head_width), bf),
            dma((4, groups)),
            dma((heads_dev,)),
            dma((heads_dev,)),
            dma,
        ],
        compiler_params=pltpu.CompilerParams(vmem_limit_bytes=60 * 1024 * 1024),
        name="mix",
    )(
        tokens,
        mix_gain.reshape(1, width),
        decay_floor.reshape(heads_dev, head_dim),
        head_gain.reshape(1, head_dim),
        route_ids.T,
        route_logits.T,
        *weights,
        prev_state,
        w_output,
    )


def on_device(
    tokens,
    mix_gain,
    w_query,
    w_forget,
    w_input,
    w_outgate,
    decay_floor,
    head_gain,
    prev_state,
    w_output,
    moe_gain,
    route_ids,
    route_logits,
    w_exp_gate,
    w_exp_up,
    w_exp_down,
):
    experts = lax.axis_size("ep") // 2
    partial_mix, coef, new_state = mix(
        tokens,
        mix_gain,
        decay_floor,
        head_gain,
        route_ids,
        route_logits,
        (w_query, w_forget, w_input, w_outgate),
        prev_state,
        w_output,
        experts,
    )
    layer_out = moe(tokens, partial_mix, moe_gain, coef, w_exp_gate, w_exp_up, w_exp_down)
    return (layer_out, new_state)


def solution(mesh):
    placed = (
        P("ep", None),
        P(),
        P(None, "tp"),
        P(None, "tp"),
        P(None, "tp"),
        P(None, "tp"),
        P("tp"),
        P(),
        P("ep", "tp", None, None),
        P("tp", None),
        P(),
        P("ep", None),
        P("ep", None),
        P("ep", None, "tp"),
        P("ep", None, "tp"),
        P("ep", "tp", None),
    )
    return jax.shard_map(
        on_device,
        mesh=mesh,
        in_specs=placed,
        out_specs=(P("ep", None), P("ep", "tp", None, None)),
        check_vma=False,
    )
```

```python
import functools

import jax
import jax.numpy as jnp
from jax import lax
from jax.experimental import pallas as pl
from jax.experimental.pallas import tpu as pltpu
from jax.sharding import PartitionSpec as P

epsilon = 1e-06
LANES = 128
MESH = pl.DeviceIdType.MESH


def rms_scale(values, gains):
    return values * lax.rsqrt(jnp.mean(values * values, axis=-1, keepdims=True) + epsilon) * gains


def line_size(ep_size):
    size = 1
    while size * size * size < ep_size:
        size *= 2
    return size


def moe_kernel(
    line,
    plane,
    tokens,
    partial_mix,
    moe_gain,
    coef,
    gate_hbm,
    up_hbm,
    down_hbm,
    out,
    other_mix,
    middle,
    rows_all,
    w_gate,
    w_up,
    w_down,
    activated,
    row_weight,
    own_half,
    pair_send,
    pair_recv,
    plane_send,
    plane_recv,
    line_send,
    line_recv,
    final_half,
    w_sems,
    mix_sems,
    ag_line_send,
    ag_line_recv,
    ag_plane_send,
    ag_plane_recv,
    ag_pair_send,
    ag_pair_recv,
    rs_pair_send,
    rs_pair_recv,
    rs_plane_send,
    rs_plane_recv,
    rs_line_send,
    rs_line_recv,
    final_sems,
):
    ep_size = line * plane
    experts = ep_size // 2
    seq_dev, width = tokens.shape
    half = width // 2
    hidden = w_gate.shape[1]
    me = lax.axis_index("ep")
    core = lax.axis_index("tp")
    peer = 1 - core
    z = me // plane
    q = me % plane

    loads = [
        pltpu.make_async_copy(gate_hbm.at[0], w_gate, w_sems.at[0]),
        pltpu.make_async_copy(up_hbm.at[0], w_up, w_sems.at[1]),
        pltpu.make_async_copy(down_hbm.at[0, :, pl.ds(0, half)], w_down.at[0], w_sems.at[2]),
        pltpu.make_async_copy(down_hbm.at[0, :, pl.ds(half, half)], w_down.at[1], w_sems.at[3]),
    ]

    upper = (2 * z) // line

    def hop(k):
        return upper * k + (1 - upper) * ((line - k) % line)

    def at_line(k):
        return ((z + hop(k)) % line) * plane + q

    def at_plane(p):
        return z * plane + (q + p) % plane

    barrier = pltpu.get_barrier_semaphore()
    pl.semaphore_signal(barrier, inc=1, device_id=(me, peer), device_id_type=MESH)
    for dz in range(1, line):
        pl.semaphore_signal(barrier, inc=1, device_id=(at_line(dz), core), device_id_type=MESH)
    for p in range(1, plane):
        pl.semaphore_signal(barrier, inc=1, device_id=(at_plane(p), core), device_id_type=MESH)
    pl.semaphore_wait(barrier, line + plane - 1)

    def remote(src, dst, send, recv, where):
        return pltpu.make_async_remote_copy(
            src_ref=src, dst_ref=dst, send_sem=send, recv_sem=recv, device_id=where, device_id_type=MESH
        )

    mix_copy = remote(partial_mix, other_mix, mix_sems.at[0], mix_sems.at[1], (me, peer))
    mix_copy.start()

    mix_copy.wait()
    mixed = partial_mix[...].astype(jnp.float32) + other_mix[...].astype(jnp.float32)
    mid = (tokens[...].astype(jnp.float32) + mixed).astype(jnp.bfloat16).astype(jnp.float32)
    middle[0] = mid[:, :half]
    middle[1] = mid[:, half:]
    normed = rms_scale(mid, moe_gain[...]).astype(jnp.bfloat16)
    rows_all[0, me, :, :half] = normed[:, :half]
    rows_all[1, me, :, :half] = normed[:, half:]
    for c in range(2):
        rows_all[c, me, :, half:] = coef[...]

    line_copies = []
    for dz in range(1, line):
        block = rows_all.at[core, me]
        index = hop(dz)
        cp = remote(block, block, ag_line_send.at[index], ag_line_recv.at[index], (at_line(dz), core))
        cp.start()
        line_copies.append((dz, cp))
    line_of = dict(line_copies)
    for load in loads:
        load.start()
    plane_copies = {}
    pair_copies = {}

    def hand_over(p, dz):
        source = ((z - hop(dz) + line) % line) * plane + (q - p + plane) % plane
        block = rows_all.at[core, source]
        cp = remote(block, block, ag_pair_send.at[p, dz], ag_pair_recv.at[p, dz], (me, peer))
        cp.start()
        pair_copies[p, dz] = cp

    for dz in range(line):
        if dz:
            line_of[dz].wait_recv()
        block = rows_all.at[core, ((z - hop(dz) + line) % line) * plane + q]
        for p in range(1, plane):
            cp = remote(
                block, block, ag_plane_send.at[p, dz], ag_plane_recv.at[p, dz], (at_plane(p), core)
            )
            cp.start()
            plane_copies[p, dz] = cp
        if dz:
            hand_over(0, dz)
    for dz in range(line):
        for p in range(1, plane):
            plane_copies[p, dz].wait_recv()
            hand_over(p, dz)
    for load in loads[:2]:
        load.wait()
    for key in pair_copies:
        pair_copies[key].wait_recv()

    total = ep_size * seq_dev
    chunk = min(total, 256)
    devs = chunk // seq_dev
    tile = 256 if hidden % 256 == 0 else hidden
    expert = me // 2

    @pl.loop(0, total // chunk)
    def _(m):
        rows = pl.ds(pl.multiple_of(m * chunk, chunk), chunk)
        who = pl.ds(m * devs, devs)
        sent = rows_all[0, who, :, half:].reshape(chunk, LANES).astype(jnp.float32)
        at = lax.broadcasted_iota(jnp.int32, (chunk, LANES), 1)
        picked = jnp.where((at == expert) | (at == expert + experts), sent, 0.0)
        row_weight[rows, :] = jnp.broadcast_to(
            jnp.sum(picked, axis=1, keepdims=True), (chunk, LANES)
        )

        @pl.loop(0, hidden // tile)
        def _(n):
            cols = pl.ds(pl.multiple_of(n * tile, tile), tile)
            left = rows_all[0, who, :, :half].reshape(chunk, half)
            right = rows_all[1, who, :, :half].reshape(chunk, half)
            gate = jnp.dot(left, w_gate[:half, cols], preferred_element_type=jnp.float32)
            gate += jnp.dot(right, w_gate[half:, cols], preferred_element_type=jnp.float32)
            up = jnp.dot(left, w_up[:half, cols], preferred_element_type=jnp.float32)
            up += jnp.dot(right, w_up[half:, cols], preferred_element_type=jnp.float32)
            activated[rows, cols] = (jax.nn.silu(gate) * up).astype(jnp.bfloat16)

    for load in loads[2:]:
        load.wait()
    step = 256 if half % 256 == 0 else half

    def down(which, store):
        @pl.loop(0, total // chunk)
        def _(m):
            rows = pl.ds(pl.multiple_of(m * chunk, chunk), chunk)
            who = pl.ds(m * devs, devs)

            @pl.loop(0, half // step)
            def _(n):
                cols = pl.ds(pl.multiple_of(n * step, step), step)
                value = jnp.dot(
                    activated[rows, :], w_down[which, :, cols], preferred_element_type=jnp.float32
                )
                value = value * row_weight[rows, 0:1]
                store[who, :, cols] = value.reshape(devs, seq_dev, step).astype(store.dtype)

    down(peer, pair_send)
    rs_pair = {}
    order = list(range(1, line)) + [0]
    for dz in order:
        part = pl.ds(((z + hop(dz)) % line) * plane, plane)
        cp = remote(
            pair_send.at[part], pair_recv.at[part], rs_pair_send.at[dz], rs_pair_recv.at[dz], (me, peer)
        )
        cp.start()
        rs_pair[dz] = cp
    down(core, own_half)

    rs_plane = {}
    for dz in order:
        first = ((z + hop(dz)) % line) * plane
        part = pl.ds(first, plane)
        rs_pair[dz].wait_recv()
        joined = own_half[part] + pair_recv[part].astype(jnp.float32)
        own_half[part] = joined
        plane_send[dz] = joined.astype(jnp.bfloat16)
        for p in range(1, plane):
            cp = remote(
                plane_send.at[dz, (q + p) % plane],
                plane_recv.at[dz, p],
                rs_plane_send.at[p, dz],
                rs_plane_recv.at[p, dz],
                (at_plane(p), core),
            )
            cp.start()
            rs_plane[p, dz] = cp
    rs_line = {}
    kept = None
    for dz in order:
        block = own_half[((z + hop(dz)) % line) * plane + q]
        for p in range(1, plane):
            rs_plane[p, dz].wait_recv()
            block = block + plane_recv[dz, p].astype(jnp.float32)
        if dz:
            line_send[dz] = block.astype(jnp.bfloat16)
            cp = remote(
                line_send.at[dz],
                line_recv.at[hop(dz)],
                rs_line_send.at[hop(dz)],
                rs_line_recv.at[hop(dz)],
                (at_line(dz), core),
            )
            cp.start()
            rs_line[dz] = cp
        else:
            kept = block
    for dz in range(1, line):
        rs_line[dz].wait_recv()
        kept = kept + line_recv[hop(dz)].astype(jnp.float32)
    final_half[core] = (middle[core] + kept).astype(jnp.bfloat16)
    last = remote(
        final_half.at[core], final_half.at[core], final_sems.at[0], final_sems.at[1], (me, peer)
    )
    last.start()
    for copies in (line_of, plane_copies, pair_copies, rs_pair, rs_plane, rs_line):
        for key in copies:
            copies[key].wait_send()
    last.wait()
    out[:, :half] = final_half[0]
    out[:, half:] = final_half[1]


def moe(tokens, partial_mix, moe_gain, coef, w_gate, w_up, w_down):
    seq_dev, width = tokens.shape
    half = width // 2
    hidden = w_gate.shape[2]
    ep_size = lax.axis_size("ep")
    line = line_size(ep_size)
    plane = ep_size // line
    bf, f32 = jnp.bfloat16, jnp.float32
    dma = pltpu.SemaphoreType.DMA
    vmem = pl.BlockSpec(memory_space=pltpu.VMEM)
    hbm = pl.BlockSpec(memory_space=pl.ANY)
    return pl.pallas_call(
        functools.partial(moe_kernel, line, plane),
        out_shape=jax.ShapeDtypeStruct((seq_dev, width), bf),
        in_specs=[vmem] * 4 + [hbm] * 3,
        out_specs=vmem,
        scratch_shapes=[
            pltpu.VMEM((seq_dev, width), bf),
            pltpu.VMEM((2, seq_dev, half), f32),
            pltpu.VMEM((2, ep_size, seq_dev, half + LANES), bf),
            pltpu.VMEM((width, hidden), bf),
            pltpu.VMEM((width, hidden), bf),
            pltpu.VMEM((2, hidden, half), bf),
            pltpu.VMEM((ep_size * seq_dev, hidden), bf),
            pltpu.VMEM((ep_size * seq_dev, LANES), f32),
            pltpu.VMEM((ep_size, seq_dev, half), f32),
            pltpu.VMEM((ep_size, seq_dev, half), bf),
            pltpu.VMEM((ep_size, seq_dev, half), bf),
            pltpu.VMEM((line, plane, seq_dev, half), bf),
            pltpu.VMEM((line, plane, seq_dev, half), bf),
            pltpu.VMEM((line, seq_dev, half), bf),
            pltpu.VMEM((line, seq_dev, half), bf),
            pltpu.VMEM((2, seq_dev, half), bf),
            dma((4,)),
            dma((2,)),
            dma((line,)),
            dma((line,)),
            dma((plane, line)),
            dma((plane, line)),
            dma((plane, line)),
            dma((plane, line)),
            dma((line,)),
            dma((line,)),
            dma((plane, line)),
            dma((plane, line)),
            dma((line,)),
            dma((line,)),
            dma((2,)),
        ],
        compiler_params=pltpu.CompilerParams(
            collective_id=0, has_side_effects=True, vmem_limit_bytes=60 * 1024 * 1024
        ),
        name="moe",
    )(tokens, partial_mix, moe_gain.reshape(1, width), coef, w_gate, w_up, w_down)


def mix_kernel(
    experts,
    tokens,
    mix_gain,
    floors,
    head_gain,
    ids,
    logits,
    query_hbm,
    forget_hbm,
    input_hbm,
    outgate_hbm,
    prev_hbm,
    output_hbm,
    partial_mix,
    coef,
    state_hbm,
    weights,
    state,
    w_output,
    total,
    w_sems,
    in_sems,
    out_sems,
    last_sem,
):
    groups = weights.shape[1]
    span = weights.shape[3]
    seq_dev = tokens.shape[0]
    heads_dev, head_dim = floors.shape
    per_group = heads_dev // groups
    loads, states, stores = {}, [], []
    for g in range(groups):
        cols = pl.ds(g * span, span)
        for n, source in enumerate((forget_hbm, query_hbm, input_hbm, outgate_hbm)):
            loads[n, g] = pltpu.make_async_copy(source.at[:, cols], weights.at[n, g], w_sems.at[n, g])
            loads[n, g].start()
    for g in range(groups):
        for h in range(g * per_group, (g + 1) * per_group):
            cp = pltpu.make_async_copy(prev_hbm.at[:, h], state.at[h], in_sems.at[h])
            cp.start()
            states.append(cp)
            stores.append(pltpu.make_async_copy(state.at[h], state_hbm.at[:, h], out_sems.at[h]))
    last = pltpu.make_async_copy(output_hbm, w_output, last_sem)
    last.start()

    slot = lax.broadcasted_iota(jnp.int32, (LANES, seq_dev), 0)
    named = slot % experts
    share = jax.nn.sigmoid(logits[0:1, :] - logits[1:2, :])
    share_two = jax.nn.sigmoid(logits[1:2, :] - logits[0:1, :])
    value = jnp.where(ids[0:1, :] == named, share, 0.0) + jnp.where(ids[1:2, :] == named, share_two, 0.0)
    high = value.astype(jnp.bfloat16).astype(jnp.float32)
    value = jnp.where(slot < experts, high, value - high)
    value = jnp.where(slot < 2 * experts, value, 0.0)
    value = jnp.concatenate([value, jnp.zeros((LANES, LANES - seq_dev), jnp.float32)], axis=1)
    coef[...] = value.T[:seq_dev].astype(jnp.bfloat16)

    normed = rms_scale(tokens[...].astype(jnp.float32), mix_gain[...]).astype(jnp.bfloat16)
    fill = jnp.zeros((head_dim - 2 * seq_dev, head_dim), jnp.float32)

    def project(g):
        return [jnp.dot(normed, weights[n, g], preferred_element_type=jnp.float32) for n in range(4)]

    for n in range(4):
        loads[n, 0].wait()
    ready = project(0)
    for g in range(groups):
        forget_pre, query, inputs, outgate_pre = ready
        for k in range(per_group):
            states[g * per_group + k].wait()
        if g + 1 < groups:
            for n in range(4):
                loads[n, g + 1].wait()
            ready = project(g + 1)
        for k in range(per_group):
            h = g * per_group + k
            cut = slice(k * head_dim, (k + 1) * head_dim)
            floor = floors[h : h + 1, :]
            forget = floor + (1.0 - floor) * jax.nn.sigmoid(forget_pre[:, cut])
            turned = jnp.concatenate([forget, query[:, cut], fill], axis=0).T
            rows = []
            for s in range(seq_dev):
                kept = jnp.broadcast_to(turned[:, s : s + 1], (head_dim, head_dim))
                fresh = kept * state[h, s] + (1.0 - kept) * inputs[s : s + 1, cut]
                state[h, s] = fresh
                asked = turned[:, seq_dev + s : seq_dev + s + 1]
                rows.append(jnp.sum(asked * fresh, axis=0, keepdims=True))
            read = jnp.concatenate(rows, axis=0)
            stores[h].start()
            gated = rms_scale(read, head_gain[...]) * jax.nn.silu(outgate_pre[:, cut])
            total[:, h * head_dim : (h + 1) * head_dim] = gated.astype(jnp.bfloat16)
    last.wait()
    partial_mix[...] = jnp.dot(
        total[...], w_output[...], preferred_element_type=jnp.float32
    ).astype(jnp.bfloat16)
    for store in stores:
        store.wait()


def mix(
    tokens, mix_gain, decay_floor, head_gain, route_ids, route_logits, weights, prev_state, w_output, experts
):
    seq_dev, width = tokens.shape
    _, heads_dev, head_dim, _ = prev_state.shape
    head_width = heads_dev * head_dim
    groups = heads_dev
    bf, f32 = jnp.bfloat16, jnp.float32
    dma = pltpu.SemaphoreType.DMA
    vmem = pl.BlockSpec(memory_space=pltpu.VMEM)
    hbm = pl.BlockSpec(memory_space=pl.ANY)
    return pl.pallas_call(
        functools.partial(mix_kernel, experts),
        out_shape=(
            jax.ShapeDtypeStruct((seq_dev, width), bf),
            jax.ShapeDtypeStruct((seq_dev, LANES), bf),
            jax.ShapeDtypeStruct(prev_state.shape, f32),
        ),
        in_specs=[vmem] * 6 + [hbm] * 6,
        out_specs=(vmem, vmem, hbm),
        scratch_shapes=[
            pltpu.VMEM((4, groups, width, head_width // groups), bf),
            pltpu.VMEM((heads_dev, seq_dev, head_dim, head_dim), f32),
            pltpu.VMEM((head_width, width), bf),
            pltpu.VMEM((seq_dev, head_width), bf),
            dma((4, groups)),
            dma((heads_dev,)),
            dma((heads_dev,)),
            dma,
        ],
        compiler_params=pltpu.CompilerParams(vmem_limit_bytes=60 * 1024 * 1024),
        name="mix",
    )(
        tokens,
        mix_gain.reshape(1, width),
        decay_floor.reshape(heads_dev, head_dim),
        head_gain.reshape(1, head_dim),
        route_ids.T,
        route_logits.T,
        *weights,
        prev_state,
        w_output,
    )


def on_device(
    tokens,
    mix_gain,
    w_query,
    w_forget,
    w_input,
    w_outgate,
    decay_floor,
    head_gain,
    prev_state,
    w_output,
    moe_gain,
    route_ids,
    route_logits,
    w_exp_gate,
    w_exp_up,
    w_exp_down,
):
    experts = lax.axis_size("ep") // 2
    partial_mix, coef, new_state = mix(
        tokens,
        mix_gain,
        decay_floor,
        head_gain,
        route_ids,
        route_logits,
        (w_query, w_forget, w_input, w_outgate),
        prev_state,
        w_output,
        experts,
    )
    layer_out = moe(tokens, partial_mix, moe_gain, coef, w_exp_gate, w_exp_up, w_exp_down)
    return (layer_out, new_state)


def solution(mesh):
    placed = (
        P("ep", None),
        P(),
        P(None, "tp"),
        P(None, "tp"),
        P(None, "tp"),
        P(None, "tp"),
        P("tp"),
        P(),
        P("ep", "tp", None, None),
        P("tp", None),
        P(),
        P("ep", None),
        P("ep", None),
        P("ep", None, "tp"),
        P("ep", None, "tp"),
        P("ep", "tp", None),
    )
    return jax.shard_map(
        on_device,
        mesh=mesh,
        in_specs=placed,
        out_specs=(P("ep", None), P("ep", "tp", None, None)),
        check_vma=False,
    )
```
